32 devices in a mesh: sp: 8 (over z, x), tp: 4 (over y, core).
Axes of the slice: x: 2, y: 2, z: 4, core: 2. Of those that a mesh axis runs over, the one named last changes fastest.
Arguments:
- query_a: bfloat16 [1024, 2048], P('sp', 'tp'), may hold values from -6 to 6
- key_a: bfloat16 [1024, 2048], P('sp', 'tp'), may hold values from -6 to 6
- value_a: bfloat16 [1024, 4096], P('sp', 'tp'), may hold values from -6 to 6
- query_b: bfloat16 [1024, 2048], P('sp', 'tp'), may hold values from -6 to 6
- key_b: bfloat16 [1024, 2048], P('sp', 'tp'), may hold values from -6 to 6
- value_b: bfloat16 [1024, 2048], P('sp', 'tp'), may hold values from -6 to 6
- in_gate: float32 [2, 2, 16, 1024], P(None, None, 'tp', 'sp'), may hold values from -6 to 300
- forget_gate: float32 [2, 2, 16, 1024], P(None, None, 'tp', 'sp'), may hold values from 0 to 14.1
- head_gain_a: float32 [16, 256], P('tp'), may hold values from 0.1 to 1.9
- head_gain_b: float32 [16, 128], P('tp'), may hold values from 0.1 to 1.9
- out_weight_a: bfloat16 [4096, 2048], P('tp'), may hold values from -0.078125 to 0.078125
- out_weight_b: bfloat16 [2048, 2048], P('tp'), may hold values from -0.078125 to 0.078125
- residual: bfloat16 [2048, 1024], P('tp', 'sp'), may hold values from -40 to 40
- norm_gain: float32 [2048], P('tp'), may hold values from 0.1 to 1.9
- routes: int32 [1024, 2], P('sp'), may hold values from 0 to 7, all different within a row; in each aligned block of 128 rows (0 to 127, 128 to 255, ...) at most 64 rows name the same one
- route_weights: float32 [1024, 2], P('sp'), may hold values from 0.2 to 1
- expert_gate: bfloat16 [8, 2048, 4096], P('sp', None, 'tp'), may hold values from -0.125 to 0.125
- expert_up: bfloat16 [8, 2048, 4096], P('sp', None, 'tp'), may hold values from -0.125 to 0.125
- expert_down: bfloat16 [8, 4096, 2048], P('sp', 'tp'), may hold values from -0.09375 to 0.09375
Outputs:
- layer_output: bfloat16 [2048, 1024], P('tp', 'sp')
The draws below stay inside these ranges and needn't reach their ends.
Inputs may be any that keep to these rules, and one draw needn't show every extreme that they name: `routes`: each row names 2 different experts. In each aligned block of 128 rows (the rows of one index of sp) no expert is named by more than 64 rows, a bound that some blocks reach.
All inputs are finite; a program needn't handle non-finite values.
Results may differ from the reference program's by a relative error of at most 0.012.
Values may be sent and summed in bfloat16 or wider, within the bound.
No kernel may reach another device: no remote copies, remote signals or barrier semaphores. Data moves between devices by JAX's collectives and lax.ppermute only.
A program may use at most 128 MiB of HBM per device.

```python
import math
import jax
import jax.numpy as jnp
import numpy as np
from jax import lax

D = 2048
HEAD_TOTAL = 16
DK = 128
DVA = 256
DVB = 128
BLOCK = 128
FF = 4096
TOP = 2
TOK_DEV = 128
TOKEN_TOTAL = 1024
EXPERTS = 8
SLOTS = 64
N_SP = 8
N_TP = 4


def draw_in_gate(key, part):
    base_key = jax.random.fold_in(key, 101)
    shape = (2, 2, HEAD_TOTAL, TOKEN_TOTAL)
    values = jax.random.uniform(base_key, shape, jnp.float32, -6.0, 0.0)
    return values


def draw_forget_gate(key, part):
    kind_key = jax.random.fold_in(key, 201)
    noise_key = jax.random.fold_in(key, 202)
    span_key = jax.random.fold_in(key, 203)
    spike_random_key = jax.random.fold_in(key, 204)
    depth_key = jax.random.fold_in(key, 205)
    shape = (2, 2, HEAD_TOTAL, TOKEN_TOTAL)
    spans = TOKEN_TOTAL // TOK_DEV
    quick = jax.random.randint(kind_key, (2, 2, HEAD_TOTAL, 1), 0, 2) == 1
    base = jnp.where(quick, 3.5, 11.0)
    offset = jax.random.uniform(span_key, (2, 2, HEAD_TOTAL, spans, 1), jnp.float32, -0.7, 0.7)
    offset = jnp.broadcast_to(offset, (2, 2, HEAD_TOTAL, spans, TOK_DEV)).reshape(shape)
    noise = jnp.clip(0.8 * jax.random.normal(noise_key, shape, jnp.float32), -2.4, 2.4)
    values = base + offset + noise
    spike_location = jax.random.randint(spike_random_key, (2, 2, HEAD_TOTAL, 3), 0, TOKEN_TOTAL)
    token_positions = jnp.arange(TOKEN_TOTAL, dtype=jnp.int32)
    spiked_rows = jnp.any(token_positions[None, None, None, :, None] == spike_location[:, :, :, None, :], axis=-1)
    depth = jax.random.uniform(depth_key, shape, jnp.float32, 0.0, 1.4)
    return jnp.where(spiked_rows & jnp.logical_not(quick), depth, values)


def draw_residual(key, part):
    noise_key = jax.random.fold_in(key, 301)
    scale_key = jax.random.fold_in(key, 302)
    fractions = jnp.arange(D, dtype=jnp.float32) / D
    token_scale = jnp.exp(jax.random.uniform(scale_key, (1, TOKEN_TOTAL), jnp.float32, math.log(0.3), math.log(3.0)))
    feature_scale = jnp.power(10.0, fractions - 0.5)
    values = jnp.clip(jax.random.normal(noise_key, (D, TOKEN_TOTAL), jnp.float32), -4.0, 4.0)
    return (values * feature_scale[:, None] * token_scale).astype(jnp.bfloat16)


def shard_levels(rng, extent, cuts, least, largest):
    gain = 1.0
    for axis_at, blocks in cuts:
        heights = jax.random.uniform(jax.random.fold_in(jax.random.fold_in(rng, 6), axis_at), (blocks,), jnp.float32, least / len(cuts), largest / len(cuts))
        gain = gain * jnp.repeat(jnp.exp(heights), extent[axis_at] // blocks).reshape((-1,) + (1,) * (len(extent) - 1 - axis_at))
    return gain


def deal_out(key, own, number, rows, count, top, reach, skew):
    sequence = jax.random.permutation(key, count)
    packed, common = shares(count, rows * top, reach, skew, True), shares(count, rows * top, reach, skew, False)
    places = jnp.arange(count)

    def named(tallies, rotation):
        used = int((tallies > 0).sum())
        fixed = max(1, used // 4)
        passed = fixed + (places - fixed + rotation * (used - fixed)) % max(1, count - fixed)
        return jnp.zeros((count,), jnp.int32).at[sequence[jnp.where(places < fixed, places, passed)]].set(jnp.asarray(tallies, jnp.int32))

    tallies = jnp.where(number % 4 == 0, named(packed, number // 4), named(common, number - number // 4 - 1))
    mixed = jax.random.permutation(jax.random.fold_in(own, 3), count)
    source_of, receiver = mixed[0:count // 2 * 2:2], mixed[1:count // 2 * 2:2]
    margin = jnp.minimum(tallies[source_of] - 1, reach - tallies[receiver]) // 2
    margin = jnp.where((source_of == sequence[0]) | (receiver == sequence[0]) | (tallies[receiver] == 0), 0, jnp.maximum(margin, 0))
    passed = jax.random.randint(jax.random.fold_in(own, 4), (count // 2,), 0, 1 << 20) % (margin + 1)
    tallies = tallies.at[source_of].add(-passed).at[receiver].add(passed)
    labels = jnp.searchsorted(jnp.cumsum(tallies), jnp.arange(rows * top), side="right").astype(jnp.int32)
    grid = labels.reshape(top, rows).T
    grid = grid[jax.random.permutation(jax.random.fold_in(own, 1), rows)]
    rotation = jax.random.randint(jax.random.fold_in(own, 2), (rows, 1), 0, top)
    return jnp.take_along_axis(grid, (jnp.arange(top)[None, :] + rotation) % top, axis=1)


def shares(count, total, limit, lean, full):
    loads = [(1 << 20) // math.isqrt(rank ** lean) + 1 for rank in range(1, count + 1)]
    largest = limit if full else min(limit, max(-(-total // count), total * loads[0] // sum(loads)))
    least = 1 if total - largest >= count - 1 else 0
    counts, surplus = [largest] + [least] * (count - 1), total - largest - least * (count - 1)
    while surplus > 0:
        candidates = [i for i in range(1, count) if counts[i] < largest] or [i for i in range(1, count) if counts[i] < limit]
        pool, remaining = sum([loads[i] for i in candidates]), surplus
        for i in candidates:
            addition = min(limit - counts[i], max(1, remaining * loads[i] // pool), surplus)
            counts[i] = counts[i] + addition
            surplus = surplus - addition
    return np.array(counts)


def scatter_about(own_key, extent, scale, most, cuts=(), held_as=jnp.bfloat16):
    drawn = jax.random.normal(own_key, extent, jnp.float32) * scale
    if len(cuts) > 0:
        drawn = shard_levels(own_key, extent, cuts, -0.22, 0.18) * drawn
    return jnp.clip(drawn, min=-most, max=most).astype(held_as)


def setup_inputs(seed: int = 0) -> dict:
    keys = jax.random.split(jax.random.key(seed), 20)
    query_a = scatter_about(keys[0], (TOKEN_TOTAL, HEAD_TOTAL * DK), 1.0, 6.0, ((0, 8), (1, 4)))
    key_a = scatter_about(keys[1], (TOKEN_TOTAL, HEAD_TOTAL * DK), 1.0, 6.0, ((0, 8), (1, 4)))
    value_a = scatter_about(keys[2], (TOKEN_TOTAL, HEAD_TOTAL * DVA), 1.0, 6.0, ((0, 8), (1, 4)))
    query_b = scatter_about(keys[3], (TOKEN_TOTAL, HEAD_TOTAL * DK), 1.0, 6.0, ((0, 8), (1, 4)))
    key_b = scatter_about(keys[4], (TOKEN_TOTAL, HEAD_TOTAL * DK), 1.0, 6.0, ((0, 8), (1, 4)))
    value_b = scatter_about(keys[5], (TOKEN_TOTAL, HEAD_TOTAL * DVB), 1.0, 6.0, ((0, 8), (1, 4)))
    in_gate = draw_in_gate(jax.random.fold_in(keys[19], 71), 0)
    forget_gate = draw_forget_gate(jax.random.fold_in(keys[19], 71), 0)
    head_gain_a = jnp.clip(1.0 + 0.18 * jax.random.normal(keys[8], (HEAD_TOTAL, DVA), jnp.float32), 0.1, 1.9)
    head_gain_b = jnp.clip(1.0 + 0.18 * jax.random.normal(keys[9], (HEAD_TOTAL, DVB), jnp.float32), 0.1, 1.9)
    out_weight_a = scatter_about(keys[10], (HEAD_TOTAL * DVA, D), (HEAD_TOTAL * (DVA + DVB)) ** -0.5, 0.078125, ((0, 4),))
    out_weight_b = scatter_about(keys[11], (HEAD_TOTAL * DVB, D), (HEAD_TOTAL * (DVA + DVB)) ** -0.5, 0.078125, ((0, 4),))
    residual = draw_residual(jax.random.fold_in(keys[19], 71), 0)
    norm_gain = jnp.clip(1.0 + 0.18 * jax.random.normal(keys[13], (D,), jnp.float32), 0.1, 1.9)
    routes_keys = jax.random.split(jax.random.fold_in(keys[14], 1), TOKEN_TOTAL // TOK_DEV)
    routes_turns = jax.random.permutation(jax.random.fold_in(keys[14], 3), TOKEN_TOTAL // TOK_DEV)
    routes = jax.vmap(lambda own, number: deal_out(jax.random.fold_in(keys[14], 2), own, number, TOK_DEV, EXPERTS, TOP, SLOTS, 3))(routes_keys, routes_turns).reshape((TOKEN_TOTAL, TOP))
    route_weights = jnp.clip(0.2 + 0.8 * jax.random.uniform(keys[15], (TOKEN_TOTAL, TOP), jnp.float32) ** shard_levels(keys[15], (TOKEN_TOTAL, TOP), ((0, 8),), -0.2, 0.2), 0.2, 1.0)
    expert_gate = scatter_about(keys[16], (EXPERTS, D, FF), D ** -0.5, 0.125, ((0, 8), (2, 4)))
    expert_up = scatter_about(keys[17], (EXPERTS, D, FF), D ** -0.5, 0.125, ((0, 8), (2, 4)))
    expert_down = scatter_about(keys[18], (EXPERTS, FF, D), FF ** -0.5, 0.09375, ((0, 8), (1, 4)))
    return dict(query_a=query_a, key_a=key_a, value_a=value_a, query_b=query_b, key_b=key_b, value_b=value_b, in_gate=in_gate, forget_gate=forget_gate, head_gain_a=head_gain_a, head_gain_b=head_gain_b, out_weight_a=out_weight_a, out_weight_b=out_weight_b, residual=residual, norm_gain=norm_gain, routes=routes, route_weights=route_weights, expert_gate=expert_gate, expert_up=expert_up, expert_down=expert_down)


EPSILON = 1e-06

def one_direction(queries, keys_in, values_in, log_input, log_decay):
    head_count, length, width_k = queries.shape
    blocks = length // BLOCK
    lower_mask = jnp.tril(jnp.ones((BLOCK, BLOCK), dtype=bool))

    def to_blocks(tensor):
        return jnp.moveaxis(tensor.reshape(head_count, blocks, BLOCK, *tensor.shape[2:]), 1, 0)

    def block_step(carried_state, inputs_block):
        memory, normal, stabilizer = carried_state
        q_block, k_block, v_block, in_block, decay_block = inputs_block
        cumulative = jnp.cumsum(decay_block, axis=-1)
        running_log_decay = cumulative + stabilizer[:, None]
        log_weights = jnp.where(lower_mask, cumulative[:, :, None] - cumulative[:, None, :] + in_block[:, None, :], -jnp.inf)
        row_peak = jnp.maximum(running_log_decay, lax.optimization_barrier(jnp.max(log_weights, axis=-1)))
        carried_weight = jnp.exp(running_log_decay - row_peak)
        scores = jnp.einsum('htd,hsd->hts', q_block, k_block) * jnp.exp(log_weights - row_peak[:, :, None])
        rounded = lax.optimization_barrier(scores.astype(jnp.bfloat16)).astype(jnp.float32)
        numerator = carried_weight[:, :, None] * jnp.einsum('htd,hde->hte', q_block, memory) + jnp.einsum('hts,hse->hte', rounded, v_block)
        denominator = carried_weight * jnp.einsum('htd,hd->ht', q_block, normal) + lax.optimization_barrier(jnp.sum(scores, axis=-1))
        outputs = numerator / jnp.maximum(jnp.abs(denominator), jnp.exp(-row_peak))[:, :, None]
        decay_total = cumulative[:, -1]
        tail_logs = decay_total[:, None] - cumulative + in_block
        new_stabilizer = jnp.maximum(decay_total + stabilizer, lax.optimization_barrier(jnp.max(tail_logs, axis=-1)))
        keep_scale = jnp.exp(decay_total + stabilizer - new_stabilizer)
        weighted_keys = k_block * jnp.exp(tail_logs - new_stabilizer[:, None])[:, :, None]
        memory = keep_scale[:, None, None] * memory + jnp.einsum('hsd,hse->hde', weighted_keys, v_block)
        normal = keep_scale[:, None] * normal + lax.optimization_barrier(jnp.sum(weighted_keys, axis=1))
        return ((memory, normal, new_stabilizer), outputs)
    start = (jnp.zeros((head_count, width_k, values_in.shape[-1]), jnp.float32), jnp.zeros((head_count, width_k), jnp.float32), jnp.zeros((head_count,), jnp.float32))
    blocked = tuple((to_blocks(tensor) for tensor in (queries, keys_in, values_in, log_input, log_decay)))
    final_state, outputs = lax.scan(block_step, start, blocked)
    return jnp.moveaxis(outputs, 0, 1).reshape(head_count, length, -1)

def mixer_group(queries, keys_in, values_in, log_input, log_decay, head_gain):
    width_k = queries.shape[1] // HEAD_TOTAL
    width_v = values_in.shape[1] // HEAD_TOTAL
    q_heads = queries.astype(jnp.float32).reshape(TOKEN_TOTAL, HEAD_TOTAL, width_k).transpose(1, 0, 2) * width_k ** (-0.5)
    k_heads = keys_in.astype(jnp.float32).reshape(TOKEN_TOTAL, HEAD_TOTAL, width_k).transpose(1, 0, 2)
    v_heads = values_in.astype(jnp.float32).reshape(TOKEN_TOTAL, HEAD_TOTAL, width_v).transpose(1, 0, 2)
    forward = one_direction(q_heads, k_heads, v_heads, log_input[0], log_decay[0])
    backward = jnp.flip(one_direction(jnp.flip(q_heads, 1), jnp.flip(k_heads, 1), jnp.flip(v_heads, 1), jnp.flip(log_input[1], 1), jnp.flip(log_decay[1], 1)), 1)
    both = forward + backward
    scaled = both * lax.rsqrt(lax.optimization_barrier(jnp.mean(both * both, axis=-1, keepdims=True)) + EPSILON) * head_gain[:, None, :]
    return scaled.astype(jnp.bfloat16).transpose(1, 0, 2).reshape(TOKEN_TOTAL, HEAD_TOTAL * width_v)

def reference(query_a, key_a, value_a, query_b, key_b, value_b, in_gate, forget_gate, head_gain_a, head_gain_b, out_weight_a, out_weight_b, residual, norm_gain, routes, route_weights, expert_gate, expert_up, expert_down):
    log_decay = jax.nn.log_sigmoid(forget_gate)
    heads_a = mixer_group(query_a, key_a, value_a, in_gate[:, 0], log_decay[:, 0], head_gain_a)
    heads_b = mixer_group(query_b, key_b, value_b, in_gate[:, 1], log_decay[:, 1], head_gain_b)
    mix = jnp.dot(heads_a, out_weight_a, preferred_element_type=jnp.float32) + jnp.dot(heads_b, out_weight_b, preferred_element_type=jnp.float32)
    updated = residual.astype(jnp.float32) + mix.T
    squares = lax.optimization_barrier(jnp.sum(updated * updated, axis=0))
    normed = (updated * lax.rsqrt(squares / D + EPSILON)[None, :] * norm_gain[:, None]).astype(jnp.bfloat16)
    token_rows = normed.T
    flat_routes = routes.reshape(N_SP, TOK_DEV * TOP)
    hits = (flat_routes[:, :, None] == jnp.arange(EXPERTS, dtype=jnp.int32)[None, None, :]).astype(jnp.int32)
    ranks = lax.optimization_barrier(jnp.sum((jnp.cumsum(hits, axis=1) - 1) * hits, axis=2))
    token_positions = (jnp.arange(N_SP, dtype=jnp.int32)[:, None] * SLOTS + ranks).reshape(TOKEN_TOTAL, TOP).astype(jnp.int32)
    owners = jnp.broadcast_to(jnp.arange(TOKEN_TOTAL, dtype=jnp.int32)[:, None], (TOKEN_TOTAL, TOP))
    table = jnp.zeros((EXPERTS, N_SP * SLOTS), jnp.int32).at[routes, token_positions].set(owners)
    group_width = FF // N_TP

    def one_expert(inputs_expert):
        gate_matrix, up_matrix, down_matrix, row_ids = inputs_expert
        rows = jnp.take(token_rows, row_ids, axis=0)
        gate = jnp.dot(rows, gate_matrix, preferred_element_type=jnp.float32)
        upward = jnp.dot(rows, up_matrix, preferred_element_type=jnp.float32)
        hidden = (jax.nn.silu(gate) * upward).astype(jnp.bfloat16)
        pieces = jnp.einsum('rjg,jgd->jrd', hidden.reshape(-1, N_TP, group_width).astype(jnp.float32), down_matrix.reshape(N_TP, group_width, D).astype(jnp.float32))
        pieces = lax.optimization_barrier(pieces.astype(jnp.bfloat16)).astype(jnp.float32)
        return lax.optimization_barrier(jnp.sum(pieces, axis=0)).astype(jnp.bfloat16)
    expert_rows = lax.map(one_expert, (expert_gate, expert_up, expert_down, table))
    picked = expert_rows[routes, token_positions].astype(jnp.float32)
    combined = updated + lax.optimization_barrier(jnp.sum(route_weights[:, :, None] * picked, axis=1)).T
    return combined.astype(jnp.bfloat16)
```

```python
import jax
import jax.numpy as jnp
from jax import lax
from jax.experimental import pallas as pl
from jax.experimental.pallas import tpu as pltpu
from jax.sharding import PartitionSpec as P

EPSILON = 1e-06
MASKED = -1e30
HIGHEST = lax.Precision.HIGHEST


def heads_kernel(offset, queries, keys_in, values_in, source_logs, target_logs, gain, heads):
    length, width_k = queries.shape
    products = lax.dot_general(
        queries[...], keys_in[...], (((1,), (1,)), ((), ())), preferred_element_type=jnp.float32
    ) * (width_k ** (-0.5))
    target = lax.broadcasted_iota(jnp.int32, products.shape, 0) + offset[0]
    source = lax.broadcasted_iota(jnp.int32, products.shape, 1)
    weights = None
    for direction in range(2):
        reached = source <= target if direction == 0 else source >= target
        logs = jnp.where(reached, source_logs[0, direction : direction + 1, :], MASKED)
        peak = jnp.max(logs, axis=1, keepdims=True)
        scores = products * jnp.exp(logs - peak)
        denominator = jnp.sum(scores, axis=1, keepdims=True)
        floor = jnp.exp(-(target_logs[0, :, direction : direction + 1] + peak))
        scaled = scores * (1.0 / jnp.maximum(jnp.abs(denominator), floor))
        weights = scaled if weights is None else weights + scaled
    both = jnp.dot(
        weights.astype(jnp.bfloat16), values_in[...], preferred_element_type=jnp.float32
    )
    spread = lax.rsqrt(jnp.mean(both * both, axis=1, keepdims=True) + EPSILON)
    heads[...] = (both * spread * gain[0]).astype(jnp.bfloat16)


def group_heads(offset, queries, keys_in, values_in, source_logs, target_logs, gain):
    head_count = gain.shape[0]
    length, total = queries.shape[0], keys_in.shape[0]
    width_k, width_v = queries.shape[1] // head_count, gain.shape[1]
    return pl.pallas_call(
        heads_kernel,
        grid_spec=pltpu.PrefetchScalarGridSpec(
            num_scalar_prefetch=1,
            grid=(head_count,),
            in_specs=[
                pl.BlockSpec((length, width_k), lambda h, o: (0, h)),
                pl.BlockSpec((total, width_k), lambda h, o: (0, h)),
                pl.BlockSpec((total, width_v), lambda h, o: (0, h)),
                pl.BlockSpec((1, 2, total), lambda h, o: (h, 0, 0)),
                pl.BlockSpec((1, length, 2), lambda h, o: (h, 0, 0)),
                pl.BlockSpec((1, 1, width_v), lambda h, o: (h, 0, 0)),
            ],
            out_specs=pl.BlockSpec((length, width_v), lambda h, o: (0, h)),
        ),
        out_shape=jax.ShapeDtypeStruct((length, head_count * width_v), jnp.bfloat16),
    )(offset, queries, keys_in, values_in, source_logs, target_logs, gain[:, None, :])


def position_logs(in_gate, forget_gate):
    log_decay = jax.nn.log_sigmoid(forget_gate)
    gates = lax.all_gather(jnp.stack([in_gate, log_decay]), "sp")
    inputs, decays = gates[:, 0], gates[:, 1]
    count, length = decays.shape[0], decays.shape[-1]
    upper = jnp.triu(jnp.ones((length, length), jnp.float32))
    running = jnp.einsum("ndghu,ut->ndght", decays, upper, precision=HIGHEST)
    earlier = jnp.tril(jnp.ones((count, count), jnp.float32), -1)
    before = jnp.einsum("nm,mdgh->ndgh", earlier, running[..., -1], precision=HIGHEST)
    running = running + before[..., None]
    forward_sums, backward_sums = running[:, 0], running[:, 1] - decays[:, 1]
    source = jnp.stack([inputs[:, 0] - forward_sums, inputs[:, 1] + backward_sums])
    source = source.transpose(2, 3, 0, 1, 4).reshape(
        source.shape[2], source.shape[3], 2, count * length
    )
    mine = lax.axis_index("sp")
    target = jnp.stack(
        [
            lax.dynamic_index_in_dim(forward_sums, mine, 0, keepdims=False),
            -lax.dynamic_index_in_dim(backward_sums, mine, 0, keepdims=False),
        ],
        axis=-1,
    )
    return source, target


def local(
    query_a,
    key_a,
    value_a,
    query_b,
    key_b,
    value_b,
    in_gate,
    forget_gate,
    head_gain_a,
    head_gain_b,
    out_weight_a,
    out_weight_b,
    residual,
    norm_gain,
    routes,
    route_weights,
    expert_gate,
    expert_up,
    expert_down,
):
    source_logs, target_logs = position_logs(in_gate, forget_gate)
    offset = (lax.axis_index("sp") * query_a.shape[0]).astype(jnp.int32).reshape(1)
    gathered = [
        lax.all_gather(tensor, "sp", axis=0, tiled=True)
        for tensor in (key_b, value_b, key_a, value_a)
    ]
    heads_b = group_heads(
        offset, query_b, gathered[0], gathered[1], source_logs[1], target_logs[1], head_gain_b
    )
    heads_a = group_heads(
        offset, query_a, gathered[2], gathered[3], source_logs[0], target_logs[0], head_gain_a
    )
    first_term = jnp.einsum("se,ec->cs", heads_a, out_weight_a, preferred_element_type=jnp.float32)
    mix = lax.psum_scatter(
        (
            first_term
            + jnp.einsum("se,ec->cs", heads_b, out_weight_b, preferred_element_type=jnp.float32)
        ).astype(jnp.bfloat16),
        "tp",
        scatter_dimension=0,
        tiled=True,
    ).astype(jnp.float32)
    updated = residual.astype(jnp.float32) + mix
    squares = lax.psum(jnp.sum(updated * updated, axis=0), "tp")
    whole_width = residual.shape[0] * lax.axis_size("tp")
    normed = (
        updated * lax.rsqrt(squares / whole_width + EPSILON)[None, :] * norm_gain[:, None]
    ).astype(jnp.bfloat16)
    token_count = routes.shape[0]
    top_count = routes.shape[1]
    expert_count = lax.axis_size("sp") * expert_gate.shape[0]
    slot_count = 2 * token_count * top_count // expert_count
    flat_routes = routes.reshape(-1)
    hits = (flat_routes[:, None] == jnp.arange(expert_count, dtype=jnp.int32)[None, :]).astype(
        jnp.int32
    )
    ranks = jnp.sum((jnp.cumsum(hits, axis=0) - 1) * hits, axis=1)
    targets = (flat_routes * slot_count + ranks).reshape(token_count, top_count)
    slot_ids = jnp.arange(expert_count * slot_count, dtype=jnp.int32)[:, None]
    selectors = [
        (slot_ids == targets[None, :, ordering_index]).astype(jnp.bfloat16)
        for ordering_index in range(top_count)
    ]
    dispatch = selectors[0]
    ordering_index = 1
    dispatch = dispatch + selectors[ordering_index]
    buffer = jnp.einsum("ps,ds->pd", dispatch, normed, preferred_element_type=jnp.float32)
    buffer = buffer.astype(jnp.bfloat16).reshape(expert_count, slot_count, -1)
    arrived = lax.all_to_all(buffer, "sp", split_axis=0, concat_axis=0, tiled=True)
    piece = lax.all_gather(arrived, "tp", axis=2, tiled=True)
    flat_rows = piece.reshape(-1, piece.shape[-1])
    gate_rows = expert_gate[0]
    up_rows = expert_up[0]
    gate = jnp.dot(flat_rows, gate_rows, preferred_element_type=jnp.float32)
    upward = jnp.dot(flat_rows, up_rows, preferred_element_type=jnp.float32)
    hidden = (
        (jax.nn.silu(gate) * upward)
        .astype(jnp.bfloat16)
        .reshape(arrived.shape[0], arrived.shape[1], -1)
    )
    sources = hidden.shape[0]
    hidden_rows = hidden.reshape(-1, hidden.shape[-1])
    columns = expert_down[0]
    summed = lax.psum_scatter(
        jnp.einsum("rf,fc->cr", hidden_rows, columns, preferred_element_type=jnp.float32).astype(
            jnp.bfloat16
        ),
        "tp",
        scatter_dimension=0,
        tiled=True,
    ).astype(jnp.float32)
    outgoing = summed.astype(jnp.bfloat16).reshape(summed.shape[0], sources, slot_count)
    returned = lax.all_to_all(outgoing, "sp", split_axis=1, concat_axis=1, tiled=True)
    returned = returned.reshape(returned.shape[0], -1)
    combined = updated
    for ordering_index in range(top_count):
        picked = jnp.dot(returned, selectors[ordering_index], preferred_element_type=jnp.float32)
        combined = combined + route_weights[:, ordering_index][None, :] * picked
    return combined.astype(jnp.bfloat16)


def solution(mesh):
    placed = (
        P("sp", "tp"),
        P("sp", "tp"),
        P("sp", "tp"),
        P("sp", "tp"),
        P("sp", "tp"),
        P("sp", "tp"),
        P(None, None, "tp", "sp"),
        P(None, None, "tp", "sp"),
        P("tp", None),
        P("tp", None),
        P("tp", None),
        P("tp", None),
        P("tp", "sp"),
        P("tp"),
        P("sp", None),
        P("sp", None),
        P("sp", None, "tp"),
        P("sp", None, "tp"),
        P("sp", "tp", None),
    )
    return jax.shard_map(
        local, mesh=mesh, in_specs=placed, out_specs=P("tp", "sp"), check_vma=False
    )
```

```python
import jax
import jax.numpy as jnp
from jax import lax
from jax.experimental import pallas as pl
from jax.experimental.pallas import tpu as pltpu
from jax.sharding import PartitionSpec as P

EPSILON = 1e-06
MASKED = -1e30
HIGHEST = lax.Precision.HIGHEST


def swapped(tensor, axis, bit):
    count = lax.axis_size(axis)
    return lax.ppermute(tensor, axis, [(place, place ^ bit) for place in range(count)])


def pick(parts, place, dimension):
    return lax.dynamic_index_in_dim(parts, place, dimension, keepdims=False)


def scattered_sum(chunk_of, axis):
    count, mine = lax.axis_size(axis), lax.axis_index(axis)
    chunks = {place: chunk_of(mine ^ place) for place in reversed(range(count))}
    bit = 1
    while bit < count:
        for place in [place for place in chunks if place & bit]:
            sent = chunks.pop(place).astype(jnp.bfloat16)
            received = swapped(sent, axis, bit).astype(jnp.float32)
            chunks[place ^ bit] = chunks[place ^ bit] + received
        bit *= 2
    return chunks[0]


def columns_of(weights, place):
    width = weights.shape[1] // lax.axis_size("tp")
    return lax.dynamic_slice_in_dim(weights, place * width, width, 1)


def doubled(tensor, axis):
    count = lax.axis_size(axis)
    pieces = {0: tensor}
    bit = count // 2
    while bit:
        for place in sorted(pieces):
            pieces[place ^ bit] = swapped(pieces[place], axis, bit)
        bit //= 2
    return [pieces[place] for place in range(count)]


def heads_kernel(slot_sizes, *refs):
    offset, queries, source_logs, source_places, target_logs, gain = refs[:6]
    parts, heads = refs[6:-1], refs[-1]
    half = len(parts) // 2

    def slots_of(group):
        found, position = [], 0
        for size in slot_sizes:
            tile = group[position][...]
            for extra in range(1, size):
                tile = tile + group[position + extra][...]
            found.append(tile)
            position += size
        return jnp.concatenate(found, axis=0)

    length, width_k = queries.shape
    products = lax.dot_general(
        queries[...],
        slots_of(parts[half:]),
        (((1,), (1,)), ((), ())),
        preferred_element_type=jnp.float32,
    ) * (width_k ** (-0.5))
    target = lax.broadcasted_iota(jnp.int32, products.shape, 0) + offset[0]
    source = source_places[...]
    weights = None
    for direction in range(2):
        reached = source <= target if direction == 0 else source >= target
        logs = jnp.where(reached, source_logs[0, direction : direction + 1, :], MASKED)
        peak = jnp.max(logs, axis=1, keepdims=True)
        scores = products * jnp.exp(logs - peak)
        denominator = jnp.sum(scores, axis=1, keepdims=True)
        floor = jnp.exp(-(target_logs[0, :, direction : direction + 1] + peak))
        scaled = scores * (1.0 / jnp.maximum(jnp.abs(denominator), floor))
        weights = scaled if weights is None else weights + scaled
    both = jnp.dot(
        weights.astype(jnp.bfloat16), slots_of(parts[:half]), preferred_element_type=jnp.float32
    )
    spread = lax.rsqrt(jnp.mean(both * both, axis=1, keepdims=True) + EPSILON)
    heads[...] = (both * spread * gain[0]).astype(jnp.bfloat16)


def group_heads(offset, queries, slots, start, source_logs, source_places, target_logs, gain):
    head_count = gain.shape[0]
    length, total = queries.shape[0], source_places.shape[1]
    width_k, width_v = queries.shape[1] // head_count, gain.shape[1]
    value_start = start // width_v
    key_start = (start + head_count * width_v) // width_k
    pieces = [piece for slot in slots for piece in slot]
    extent = pieces[0].shape[0]
    value_spec = pl.BlockSpec((extent, width_v), lambda h, o: (0, value_start + h))
    key_spec = pl.BlockSpec((extent, width_k), lambda h, o: (0, key_start + h))
    sizes = tuple(len(slot) for slot in slots)
    return pl.pallas_call(
        lambda *refs: heads_kernel(sizes, *refs),
        grid_spec=pltpu.PrefetchScalarGridSpec(
            num_scalar_prefetch=1,
            grid=(head_count,),
            in_specs=[
                pl.BlockSpec((length, width_k), lambda h, o: (0, h)),
                pl.BlockSpec((1, 2, total), lambda h, o: (h, 0, 0)),
                pl.BlockSpec((1, total), lambda h, o: (0, 0)),
                pl.BlockSpec((1, length, 2), lambda h, o: (h, 0, 0)),
                pl.BlockSpec((1, 1, width_v), lambda h, o: (h, 0, 0)),
            ]
            + [value_spec] * len(pieces)
            + [key_spec] * len(pieces),
            out_specs=pl.BlockSpec((length, width_v), lambda h, o: (0, h)),
        ),
        out_shape=jax.ShapeDtypeStruct((length, head_count * width_v), jnp.bfloat16),
    )(
        offset,
        queries,
        source_logs,
        source_places,
        target_logs,
        gain[:, None, :],
        *pieces,
        *pieces,
    )


def gate_columns(in_gate, forget_gate):
    gates = jnp.stack([in_gate, jax.nn.log_sigmoid(forget_gate)])
    rest = gates.reshape(-1, gates.shape[-1])
    parts = []
    for _ in range(3):
        part = lax.reduce_precision(rest, 8, 7)
        parts.append(part.astype(jnp.bfloat16))
        rest = rest - part
    return jnp.concatenate(parts, axis=0).T


def position_logs(slots, blocks, mine, in_gate):
    width = 6 * in_gate[..., 0].size
    columns = [[piece[:, -width:].astype(jnp.float32) for piece in slot] for slot in slots]
    gates = jnp.concatenate([sum(slot[1:], slot[0]) for slot in columns])
    gates = gates.reshape(blocks.shape[0], in_gate.shape[-1], 3, -1).sum(axis=2)
    gates = gates.transpose(0, 2, 1).reshape((-1, 2) + in_gate.shape)
    inputs, decays = gates[:, 0], gates[:, 1]
    count, length = decays.shape[0], decays.shape[-1]
    upper = jnp.triu(jnp.ones((length, length), jnp.float32))
    running = jnp.einsum("ndghu,ut->ndght", decays, upper, precision=HIGHEST)
    earlier = (blocks[None, :] < blocks[:, None]).astype(jnp.float32)
    before = jnp.einsum("nm,mdgh->ndgh", earlier, running[..., -1], precision=HIGHEST)
    running = running + before[..., None]
    forward_sums, backward_sums = running[:, 0], running[:, 1] - decays[:, 1]
    source = jnp.stack([inputs[:, 0] - forward_sums, inputs[:, 1] + backward_sums])
    source = source.transpose(2, 3, 0, 1, 4).reshape(
        source.shape[2], source.shape[3], 2, count * length
    )
    own = jnp.argmax(blocks == mine)
    target = jnp.stack([pick(forward_sums, own, 0), -pick(backward_sums, own, 0)], axis=-1)
    return source, target


def rows_product(pieces, weights):
    mine, total = lax.axis_index("tp"), None
    height = weights.shape[0] // len(pieces)
    for place, piece in enumerate(pieces):
        part = jnp.dot(
            piece,
            lax.dynamic_slice_in_dim(weights, (mine ^ place) * height, height, 0),
            preferred_element_type=jnp.float32,
        )
        total = part if total is None else total + part
    return total


def local(
    query_a,
    key_a,
    value_a,
    query_b,
    key_b,
    value_b,
    in_gate,
    forget_gate,
    head_gain_a,
    head_gain_b,
    out_weight_a,
    out_weight_b,
    residual,
    norm_gain,
    routes,
    route_weights,
    expert_gate,
    expert_up,
    expert_down,
):
    length, mine = query_a.shape[0], lax.axis_index("sp")
    count = lax.axis_size("sp")
    offset = (mine * length).astype(jnp.int32).reshape(1)
    memory = jnp.concatenate(
        [value_a, key_a, value_b, key_b, gate_columns(in_gate, forget_gate)], axis=1
    )
    memory = lax.all_gather(memory, "sp", axis=0, tiled=True)
    blocks = jnp.arange(count, dtype=jnp.int32)
    slots = [[memory]]
    places = (blocks[:, None] * length + jnp.arange(length, dtype=jnp.int32)).reshape(1, -1)
    source_logs, target_logs = position_logs(slots, blocks, mine, in_gate)
    start_b = value_a.shape[1] + key_a.shape[1]
    heads_b = group_heads(
        offset, query_b, slots, start_b, source_logs[1], places, target_logs[1], head_gain_b
    )
    heads_a = group_heads(
        offset, query_a, slots, 0, source_logs[0], places, target_logs[0], head_gain_a
    )

    def mixed(place):
        return jnp.einsum(
            "se,ec->cs",
            heads_a,
            columns_of(out_weight_a, place),
            preferred_element_type=jnp.float32,
        ) + jnp.einsum(
            "se,ec->cs",
            heads_b,
            columns_of(out_weight_b, place),
            preferred_element_type=jnp.float32,
        )

    mix = scattered_sum(mixed, "tp")
    updated = residual.astype(jnp.float32) + mix
    squares = lax.psum(jnp.sum(updated * updated, axis=0), "tp")
    whole_width = residual.shape[0] * lax.axis_size("tp")
    normed = (
        updated * lax.rsqrt(squares / whole_width + EPSILON)[None, :] * norm_gain[:, None]
    ).astype(jnp.bfloat16)
    token_count = routes.shape[0]
    top_count = routes.shape[1]
    expert_count = lax.axis_size("sp") * expert_gate.shape[0]
    slot_count = 2 * token_count * top_count // expert_count
    flat_routes = routes.reshape(-1)
    hits = (flat_routes[:, None] == jnp.arange(expert_count, dtype=jnp.int32)[None, :]).astype(
        jnp.int32
    )
    ranks = jnp.sum((jnp.cumsum(hits, axis=0) - 1) * hits, axis=1)
    targets = (flat_routes * slot_count + ranks).reshape(token_count, top_count)
    slot_ids = jnp.arange(expert_count * slot_count, dtype=jnp.int32)[:, None]
    selectors = [
        (slot_ids == targets[None, :, ordering_index]).astype(jnp.bfloat16)
        for ordering_index in range(top_count)
    ]
    dispatch = selectors[0]
    ordering_index = 1
    dispatch = dispatch + selectors[ordering_index]
    buffer = jnp.einsum("ps,ds->pd", dispatch, normed, preferred_element_type=jnp.float32)
    buffer = buffer.astype(jnp.bfloat16).reshape(expert_count, slot_count, -1)
    arrived = lax.all_to_all(buffer, "sp", split_axis=0, concat_axis=0, tiled=True)
    pieces = doubled(arrived.reshape(-1, arrived.shape[-1]), "tp")
    gate = rows_product(pieces, expert_gate[0])
    upward = rows_product(pieces, expert_up[0])
    hidden = (
        (jax.nn.silu(gate) * upward)
        .astype(jnp.bfloat16)
        .reshape(arrived.shape[0], arrived.shape[1], -1)
    )
    sources = hidden.shape[0]
    hidden_rows = hidden.reshape(-1, hidden.shape[-1])
    columns = expert_down[0]
    summed = scattered_sum(
        lambda place: jnp.dot(
            hidden_rows, columns_of(columns, place), preferred_element_type=jnp.float32
        ),
        "tp",
    )
    outgoing = summed.astype(jnp.bfloat16).reshape(sources, slot_count, -1)
    returned = lax.all_to_all(outgoing, "sp", split_axis=0, concat_axis=0, tiled=True)
    returned = returned.reshape(-1, returned.shape[-1])
    combined = updated
    for ordering_index in range(top_count):
        picked = jnp.einsum(
            "pd,pt->dt", returned, selectors[ordering_index], preferred_element_type=jnp.float32
        )
        combined = combined + route_weights[:, ordering_index][None, :] * picked
    return combined.astype(jnp.bfloat16)


def solution(mesh):
    placed = (
        P("sp", "tp"),
        P("sp", "tp"),
        P("sp", "tp"),
        P("sp", "tp"),
        P("sp", "tp"),
        P("sp", "tp"),
        P(None, None, "tp", "sp"),
        P(None, None, "tp", "sp"),
        P("tp", None),
        P("tp", None),
        P("tp", None),
        P("tp", None),
        P("tp", "sp"),
        P("tp"),
        P("sp", None),
        P("sp", None),
        P("sp", None, "tp"),
        P("sp", None, "tp"),
        P("sp", "tp", None),
    )
    return jax.shard_map(
        local, mesh=mesh, in_specs=placed, out_specs=P("tp", "sp"), check_vma=False
    )
```
